32 devices in a mesh: dp: 4 (over y, x), kv: 4 (over z), tp: 2 (over core).
Axes of the slice: x: 2, y: 2, z: 4, core: 2. Of those that a mesh axis runs over, the one named last changes fastest.
Arguments:
- tokens: bfloat16 [64, 16, 2048], P('dp'), may hold values from -6 to 6
- norm_gain: float32 [2048], replicated, may hold values from 0.1 to 1.9
- query_weight: bfloat16 [2048, 1024], P(None, 'tp'), may hold values from -0.125 to 0.125
- key_weight: bfloat16 [2048, 256], P(None, 'tp'), may hold values from -0.125 to 0.125
- value_weight: bfloat16 [2048, 256], P(None, 'tp'), may hold values from -0.125 to 0.125
- forget_weight: bfloat16 [2048, 8], replicated, may hold values from -0.125 to 0.125
- forget_bias: float32 [8], replicated, may hold values from 0 to 4
- query_gain: float32 [128], replicated, may hold values from 0.1 to 1.9
- key_gain: float32 [128], replicated, may hold values from 0.1 to 1.9
- output_weight: bfloat16 [1024, 2048], P('tp', 'kv'), may hold values from -0.1875 to 0.1875
- cache_keys: bfloat16 [64, 1024, 2, 128], P('dp', 'kv', 'tp'), may hold values from -512 to 512
- cache_values: bfloat16 [64, 1024, 2, 128], P('dp', 'kv', 'tp'), may hold values from -6 to 6
- cache_logcum: float32 [64, 1024, 8], P('dp', 'kv', 'tp'), may hold values from -205 to 0, as said below
- pending_keys: bfloat16 [64, 4, 2, 128], P('dp', None, 'tp'), may hold values from -6 to 6
- pending_values: bfloat16 [64, 4, 2, 128], P('dp', None, 'tp'), may hold values from -6 to 6
- pending_logcum: float32 [64, 4, 8], P('dp', None, 'tp'), may hold values from -205 to 0, as said below
- lengths: int32 [64], P('dp'), may hold values from 512 to 1020, as said below
- accepted: int32 [64], P('dp'), may hold values from 1 to 4
- parents: int32 [64, 16], P('dp'), may hold values from -1 to 14, as said below
Outputs:
- result: bfloat16 [64, 16, 2048], P('dp', None, ('kv', 'tp'))
The draws below stay inside these ranges and needn't reach their ends.
Inputs may be any that keep to these rules, and one draw needn't show every extreme that they name: Positions below lengths hold a sequence's past; the last step's accepted proposals go to positions lengths to lengths + accepted - 1. `parents`: the parent of proposal i is -1 (the last accepted token) or a proposal before i. `cache_logcum`: non-increasing along positions for every sequence and head. `pending_logcum`: the cumulative log gates at positions lengths to lengths + 3, continuing cache_logcum.
All inputs are finite; a program needn't handle non-finite values.
Results may differ from the reference program's by a relative error of at most 0.014.
Values may be sent and summed in bfloat16 or wider, within the bound.
A program may use at most 128 MiB of HBM per device.

```python
import math
import jax
import jax.numpy as jnp
from jax import lax

D = 2048
HEADS = 8
KV_HEADS = 2
HEAD_DIM = 128
PROP = 16
ACC_MAX = 4
POS_DEV = 256
SEQUENCE_COUNT = 64
LEN = 1024
BLOCKS = 4
GROUPS = 2
Q_WIDTH = 1024
KV_WIDTH = 256


def gate_tables(key):
    overall_length = LEN + ACC_MAX
    lengths = jax.random.randint(jax.random.fold_in(key, 101), (SEQUENCE_COUNT,), LEN // 2, LEN - ACC_MAX + 1, dtype=jnp.int32)
    head_order = jax.random.permutation(jax.random.fold_in(key, 102), HEADS)
    fast_count = HEADS // 2
    quick_fading_heads = (head_order < fast_count).astype(jnp.float32)
    slow_rate = jnp.exp(jax.random.uniform(jax.random.fold_in(key, 103), (SEQUENCE_COUNT, 1, HEADS), jnp.float32, math.log(0.2), math.log(0.8))) / LEN
    fast_rate = jnp.exp(jax.random.uniform(jax.random.fold_in(key, 104), (SEQUENCE_COUNT, 1, HEADS), jnp.float32, math.log(0.01), math.log(1.0 / 30.0)))
    fading_speed = quick_fading_heads * fast_rate + (1.0 - quick_fading_heads) * slow_rate
    block_count = overall_length // POS_DEV + 1
    block_spread = jnp.exp(jax.random.uniform(jax.random.fold_in(key, 105), (SEQUENCE_COUNT, block_count, HEADS), jnp.float32, math.log(0.4), math.log(2.5)))
    token_place = jnp.arange(overall_length, dtype=jnp.int32)
    block_lookup = block_spread[:, token_place // POS_DEV, :]
    jaggedness = jnp.exp(jax.random.uniform(jax.random.fold_in(key, 106), (SEQUENCE_COUNT, overall_length, HEADS), jnp.float32, math.log(0.5), math.log(2.0)))
    spike_location = jax.random.randint(jax.random.fold_in(key, 107), (SEQUENCE_COUNT, 3), 0, overall_length, dtype=jnp.int32)
    spike_magnitude = jax.random.uniform(jax.random.fold_in(key, 108), (SEQUENCE_COUNT, 3), jnp.float32, 0.22, 0.6)
    spike_penalty = jnp.sum((token_place[None, None, :] == spike_location[:, :, None]).astype(jnp.float32) * spike_magnitude[:, :, None], axis=1)
    length_steps = fading_speed * block_lookup * jaggedness + spike_penalty[:, :, None] * (1.0 - quick_fading_heads)
    return (lengths, -jnp.cumsum(length_steps, axis=1))


def draw_lengths(key, part):
    lengths, cumulative = gate_tables(key)
    return lengths


def draw_cache_logcum(key, part):
    lengths, cumulative = gate_tables(key)
    return cumulative[:, :LEN, :].astype(jnp.float32)


def draw_pending_logcum(key, part):
    lengths, cumulative = gate_tables(key)
    indices = lengths[:, None] + jnp.arange(ACC_MAX, dtype=jnp.int32)[None, :]
    return jnp.take_along_axis(cumulative, indices[:, :, None], axis=1).astype(jnp.float32)


def draw_parents(key, part):
    bounds = jnp.arange(PROP, dtype=jnp.int32)[None, :]
    return jax.random.randint(key, (SEQUENCE_COUNT, PROP), -1, bounds, dtype=jnp.int32)


def draw_cache_keys(key, part):
    shape = (SEQUENCE_COUNT, LEN, KV_HEADS, HEAD_DIM)
    drawn = jnp.clip(jax.random.normal(jax.random.fold_in(key, 201), shape, jnp.float32), -6.0, 6.0)
    return drawn.astype(jnp.bfloat16)


def with_ends(values, stream_key, least, largest):
    index_at = [jax.random.randint(jax.random.fold_in(stream_key, axis), (), 0, length) for axis, length in enumerate(values.shape)]
    main_axis = values.shape.index(max(values.shape))
    next_to = index_at[:main_axis] + [(index_at[main_axis] + 1) % values.shape[main_axis]] + index_at[main_axis + 1:]
    return values.at[tuple(index_at)].set(least).at[tuple(next_to)].set(largest)


def level_of(key, extent, pieces, smallest, largest):
    gain = 1.0
    for dim, shards_of in pieces:
        heights = jax.random.uniform(jax.random.fold_in(jax.random.fold_in(key, 6), dim), (shards_of,), jnp.float32, smallest / len(pieces), largest / len(pieces))
        gain = gain * jnp.repeat(jnp.exp(heights), extent[dim] // shards_of).reshape((-1,) + (1,) * (len(extent) - 1 - dim))
    return gain


def centred(own_key, extent, width, reach, shards=(), kind=jnp.bfloat16):
    array = jax.random.normal(own_key, extent, jnp.float32) * width
    if len(shards) > 0:
        array = level_of(own_key, extent, shards, -0.22, 0.18) * array
    return jnp.clip(array, min=-reach, max=reach).astype(kind)


def setup_inputs(seed: int = 0) -> dict:
    streams_of = jax.random.split(jax.random.key(seed), 20)
    return {
        "tokens": centred(streams_of[0], (SEQUENCE_COUNT, PROP, D), 1.0, 6.0, ((0, 4),)),
        "norm_gain": jnp.clip(1.0 + 0.18 * jax.random.normal(streams_of[1], (D,), jnp.float32), 0.1, 1.9),
        "query_weight": centred(streams_of[2], (D, Q_WIDTH), D ** -0.5, 0.125, ((1, 2),)),
        "key_weight": centred(streams_of[3], (D, KV_WIDTH), D ** -0.5, 0.125, ((1, 2),)),
        "value_weight": centred(streams_of[4], (D, KV_WIDTH), D ** -0.5, 0.125, ((1, 2),)),
        "forget_weight": centred(streams_of[5], (D, HEADS), D ** -0.5, 0.125),
        "forget_bias": jnp.clip(jax.random.uniform(streams_of[6], (HEADS,), jnp.float32, 0.0, 4.0), 0.0, 4.0),
        "query_gain": jnp.clip(1.0 + 0.18 * jax.random.normal(streams_of[7], (HEAD_DIM,), jnp.float32), 0.1, 1.9),
        "key_gain": jnp.clip(1.0 + 0.18 * jax.random.normal(streams_of[8], (HEAD_DIM,), jnp.float32), 0.1, 1.9),
        "output_weight": centred(streams_of[9], (Q_WIDTH, D), Q_WIDTH ** -0.5, 0.1875, ((0, 2), (1, 4))),
        "cache_keys": draw_cache_keys(jax.random.fold_in(streams_of[19], 71), 0),
        "cache_values": centred(streams_of[11], (SEQUENCE_COUNT, LEN, KV_HEADS, HEAD_DIM), 1.0, 6.0, ((0, 4), (1, 4), (2, 2))),
        "cache_logcum": draw_cache_logcum(jax.random.fold_in(streams_of[19], 71), 0),
        "pending_keys": centred(streams_of[13], (SEQUENCE_COUNT, ACC_MAX, KV_HEADS, HEAD_DIM), 1.0, 6.0, ((0, 4), (2, 2))),
        "pending_values": centred(streams_of[14], (SEQUENCE_COUNT, ACC_MAX, KV_HEADS, HEAD_DIM), 1.0, 6.0, ((0, 4), (2, 2))),
        "pending_logcum": draw_pending_logcum(jax.random.fold_in(streams_of[19], 71), 0),
        "lengths": draw_lengths(jax.random.fold_in(streams_of[19], 71), 0),
        "accepted": with_ends(jax.random.randint(streams_of[17], (SEQUENCE_COUNT,), 1, ACC_MAX + 1), jax.random.fold_in(streams_of[17], 1), 1, ACC_MAX).astype(jnp.int32),
        "parents": draw_parents(jax.random.fold_in(streams_of[19], 71), 0),
    }


EPSILON = 1e-06
NEG_LARGE = -1e+30
HIGHEST = lax.Precision.HIGHEST

def head_norm(vectors, gain_vec):
    return vectors * lax.rsqrt(lax.optimization_barrier(jnp.mean(vectors * vectors, axis=-1, keepdims=True)) + EPSILON) * gain_vec

def ancestors(parents):
    node_count = parents.shape[-1]
    indices = jnp.arange(node_count, dtype=jnp.int32)
    reachable = (parents[..., None] == indices).astype(jnp.float32) + jnp.eye(node_count, dtype=jnp.float32)
    for doubling in range((node_count - 1).bit_length()):
        reachable = jnp.minimum(jnp.einsum('sij,sjk->sik', reachable, reachable, precision=HIGHEST), 1.0)
    return reachable

def one_sequence(inputs):
    query_rows, key_rows, value_rows, cumulative, ancestry, cache_k, cache_v, cache_l, pend_k, pend_v, pend_l, length_now, taken_now = inputs
    sharing = HEADS // KV_HEADS
    scaling = HEAD_DIM ** (-0.5)
    token_place = jnp.arange(LEN, dtype=jnp.int32)
    offset = token_place - length_now
    inserted = (offset >= 0) & (offset < taken_now)
    one_hot = ((offset[:, None] == jnp.arange(ACC_MAX, dtype=jnp.int32)[None, :]) & inserted[:, None]).astype(jnp.float32)
    all_keys = jnp.where(inserted[:, None, None], jnp.einsum('la,akd->lkd', one_hot, pend_k.astype(jnp.float32), precision=HIGHEST), cache_k.astype(jnp.float32))
    all_values = jnp.where(inserted[:, None, None], jnp.einsum('la,akd->lkd', one_hot, pend_v.astype(jnp.float32), precision=HIGHEST), cache_v.astype(jnp.float32))
    all_logcum = jnp.where(inserted[:, None], jnp.einsum('la,ah->lh', one_hot, pend_l, precision=HIGHEST), cache_l)
    usable = token_place < length_now + taken_now
    query_group = query_rows.astype(jnp.float32).reshape(PROP, KV_HEADS, sharing, HEAD_DIM)
    scores = jnp.einsum('pkgd,lkd->kgpl', query_group, all_keys, precision=HIGHEST).reshape(HEADS, PROP, LEN)
    scores = scores * scaling + cumulative.T[:, :, None] - all_logcum.T[:, None, :]
    blocked = scores.reshape(HEADS, PROP, BLOCKS, POS_DEV)
    visible = usable.reshape(BLOCKS, POS_DEV)[None, None]
    block_max = lax.optimization_barrier(jnp.max(jnp.where(visible, blocked, NEG_LARGE), axis=-1))
    weights = jnp.where(visible, jnp.exp(blocked - block_max[..., None]), 0.0)
    block_sum = lax.optimization_barrier(jnp.sum(weights, axis=-1))
    rounded = lax.optimization_barrier(weights.astype(jnp.bfloat16)).astype(jnp.float32)
    rounded = rounded.reshape(KV_HEADS, sharing, PROP, BLOCKS, POS_DEV)
    block_values = jnp.einsum('kgpnl,nlkd->kgpnd', rounded, all_values.reshape(BLOCKS, POS_DEV, KV_HEADS, HEAD_DIM), precision=HIGHEST)
    block_values = block_values.reshape(HEADS, PROP, BLOCKS, HEAD_DIM)
    tree_scores = jnp.einsum('pkgd,jkd->kgpj', query_group, key_rows.astype(jnp.float32), precision=HIGHEST).reshape(HEADS, PROP, PROP)
    tree_scores = tree_scores * scaling + cumulative.T[:, :, None] - cumulative.T[:, None, :]
    tree_mask = ancestry[None] > 0.5
    tree_max = lax.optimization_barrier(jnp.max(jnp.where(tree_mask, tree_scores, NEG_LARGE), axis=-1))
    tree_weights = jnp.where(tree_mask, jnp.exp(tree_scores - tree_max[..., None]), 0.0)
    tree_sum = lax.optimization_barrier(jnp.sum(tree_weights, axis=-1))
    tree_rounded = lax.optimization_barrier(tree_weights.astype(jnp.bfloat16)).astype(jnp.float32)
    tree_values = jnp.einsum('kgpj,jkd->kgpd', tree_rounded.reshape(KV_HEADS, sharing, PROP, PROP), value_rows.astype(jnp.float32), precision=HIGHEST).reshape(HEADS, PROP, HEAD_DIM)
    overall = jnp.maximum(lax.optimization_barrier(jnp.max(block_max, axis=-1)), tree_max)
    factor_cache = jnp.exp(block_max - overall[..., None])
    factor_tree = jnp.exp(tree_max - overall)
    denominator = lax.optimization_barrier(jnp.sum(block_sum * factor_cache, axis=-1)) + tree_sum * factor_tree
    numerator = lax.optimization_barrier(jnp.sum(block_values * factor_cache[..., None], axis=2)) + tree_values * factor_tree[..., None]
    return jnp.transpose(numerator / denominator[..., None], (1, 0, 2)).astype(jnp.bfloat16)

def reference(tokens, norm_gain, query_weight, key_weight, value_weight, forget_weight, forget_bias, query_gain, key_gain, output_weight, cache_keys, cache_values, cache_logcum, pending_keys, pending_values, pending_logcum, lengths, accepted, parents):
    seq_count, node_count, model_width = tokens.shape
    widened = tokens.astype(jnp.float32)
    normed = (widened * lax.rsqrt(lax.optimization_barrier(jnp.mean(widened * widened, axis=-1, keepdims=True)) + EPSILON) * norm_gain).astype(jnp.bfloat16)
    token_rows = normed.reshape(seq_count * node_count, model_width)
    query_raw = jnp.dot(token_rows, query_weight, preferred_element_type=jnp.float32)
    key_raw = jnp.dot(token_rows, key_weight, preferred_element_type=jnp.float32)
    value_raw = jnp.dot(token_rows, value_weight, preferred_element_type=jnp.float32)
    queries = head_norm(query_raw.reshape(seq_count, node_count, HEADS, HEAD_DIM), query_gain).astype(jnp.bfloat16)
    keys_new = head_norm(key_raw.reshape(seq_count, node_count, KV_HEADS, HEAD_DIM), key_gain).astype(jnp.bfloat16)
    values_new = value_raw.reshape(seq_count, node_count, KV_HEADS, HEAD_DIM).astype(jnp.bfloat16)
    log_gates = jax.nn.log_sigmoid(jnp.dot(token_rows, forget_weight, preferred_element_type=jnp.float32) + forget_bias).reshape(seq_count, node_count, HEADS)
    ancestry = ancestors(parents)
    choose = (jnp.arange(ACC_MAX, dtype=jnp.int32)[None, :] == (accepted - 1)[:, None]).astype(jnp.float32)
    base_gate = jnp.einsum('sa,sah->sh', choose, pending_logcum, precision=HIGHEST)
    cumulative = base_gate[:, None, :] + jnp.einsum('sij,sjh->sih', ancestry, log_gates, precision=HIGHEST)
    attended = lax.map(one_sequence, (queries, keys_new, values_new, cumulative, ancestry, cache_keys, cache_values, cache_logcum, pending_keys, pending_values, pending_logcum, lengths, accepted))
    grouped = attended.reshape(seq_count, node_count, GROUPS, Q_WIDTH // GROUPS).astype(jnp.float32)
    out_rows = output_weight.reshape(GROUPS, Q_WIDTH // GROUPS, model_width).astype(jnp.float32)
    head_part = jnp.einsum('spgc,gcd->gspd', grouped, out_rows, precision=HIGHEST).astype(jnp.bfloat16)
    return lax.optimization_barrier(jnp.sum(head_part.astype(jnp.float32), axis=0)).astype(jnp.bfloat16)
```

```python
import functools

import jax
import jax.numpy as jnp
from jax import lax
from jax.experimental import pallas as pl
from jax.experimental.pallas import tpu as pltpu
from jax.sharding import PartitionSpec as P

EPSILON = 1e-06
NEG_LARGE = -1e30
HIGHEST = lax.Precision.HIGHEST


def joined(shard, axis, join):
    gathered = jax.tree.map(
        lambda a, kind: lax.all_gather(a.astype(kind), axis),
        shard,
        (jnp.bfloat16, jnp.bfloat16, jnp.bfloat16),
    )

    def take(source):
        return jax.tree.map(
            lambda a, own: lax.dynamic_index_in_dim(a, source, 0, False).astype(own.dtype),
            gathered,
            shard,
        )

    return lax.fori_loop(
        1, lax.axis_size(axis), lambda source, state: join(state, take(source)), take(0)
    )


def head_norm(vectors, gain_vec):
    return (
        vectors
        * lax.rsqrt(jnp.mean(vectors * vectors, axis=-1, keepdims=True) + EPSILON)
        * gain_vec
    )


def ancestors(parents):
    node_count = parents.shape[-1]
    indices = jnp.arange(node_count, dtype=jnp.int32)
    reachable = (parents[..., None] == indices).astype(jnp.float32) + jnp.eye(
        node_count, dtype=jnp.float32
    )
    for doubling in range((node_count - 1).bit_length()):
        reachable = jnp.minimum(
            jnp.einsum("sij,sjk->sik", reachable, reachable, precision=HIGHEST), 1.0
        )
    return reachable


def join_blocks(earlier, later):
    larger = jnp.maximum(earlier[0], later[0])
    left_factor = jnp.exp(earlier[0] - larger)
    right_factor = jnp.exp(later[0] - larger)
    return (
        larger,
        earlier[1] * left_factor + later[1] * right_factor,
        earlier[2] * left_factor[..., None] + later[2] * right_factor[..., None],
    )


def to_rows(values):
    moved = jnp.swapaxes(values, 1, 2)
    return moved.reshape((moved.shape[0] * moved.shape[1],) + moved.shape[2:])


def finish_rows(cache_max, cache_sum, cache_acc, tree_max, tree_sum, tree_acc):
    overall = jnp.maximum(cache_max, tree_max)
    factor_cache = jnp.exp(cache_max - overall)
    factor_tree = jnp.exp(tree_max - overall)
    denominator = cache_sum * factor_cache + tree_sum * factor_tree
    numerator = cache_acc * factor_cache[..., None] + tree_acc * factor_tree[..., None]
    attended = (numerator / denominator[..., None]).astype(jnp.bfloat16)
    return attended.reshape(attended.shape[0], attended.shape[1] * attended.shape[2])


def shards(
    tokens,
    norm_gain,
    query_weight,
    key_weight,
    value_weight,
    forget_weight,
    forget_bias,
    query_gain,
    key_gain,
    output_weight,
    cache_keys,
    cache_values,
    cache_logcum,
    pending_keys,
    pending_values,
    pending_logcum,
    lengths,
    accepted,
    parents,
):
    seq_count, node_count, model_width = tokens.shape
    token_rows = seq_count * node_count
    head_size = query_gain.shape[0]
    query_cols = query_weight.shape[1]
    key_cols = key_weight.shape[1]
    local_heads = query_cols // head_size
    key_heads = key_cols // head_size
    sharing = local_heads // key_heads
    block_len = cache_keys.shape[1]
    most_taken = pending_keys.shape[1]
    scaling = head_size ** (-0.5)
    widened = tokens.reshape(token_rows, model_width).astype(jnp.float32)
    normed = (
        widened
        * lax.rsqrt(jnp.mean(widened * widened, axis=-1, keepdims=True) + EPSILON)
        * norm_gain
    ).astype(jnp.bfloat16)
    joined_weight = jnp.concatenate([query_weight, key_weight, value_weight], axis=1)
    summed = jnp.dot(normed, joined_weight, preferred_element_type=jnp.float32)
    query_part = head_norm(
        summed[:, :query_cols].reshape(token_rows, local_heads, head_size), query_gain
    )
    key_part = head_norm(
        summed[:, query_cols : query_cols + key_cols].reshape(token_rows, key_heads, head_size),
        key_gain,
    )
    queries = query_part.astype(jnp.bfloat16).reshape(
        seq_count, node_count, key_heads, sharing, head_size
    )
    keys_new = key_part.astype(jnp.bfloat16).reshape(seq_count, node_count, key_heads, head_size)
    values_new = (
        summed[:, query_cols + key_cols :]
        .astype(jnp.bfloat16)
        .reshape(seq_count, node_count, key_heads, head_size)
    )
    head_start = lax.axis_index("tp") * local_heads
    forget_cols = lax.dynamic_slice_in_dim(forget_weight, head_start, local_heads, 1)
    gate_bias = lax.dynamic_slice_in_dim(forget_bias, head_start, local_heads, 0)
    log_gates = jax.nn.log_sigmoid(
        jnp.dot(normed, forget_cols, preferred_element_type=jnp.float32) + gate_bias
    ).reshape(seq_count, node_count, local_heads)
    ancestry = ancestors(parents)
    choose = (jnp.arange(most_taken, dtype=jnp.int32)[None, :] == (accepted - 1)[:, None]).astype(
        jnp.float32
    )
    base_gate = jnp.einsum("sa,sah->sh", choose, pending_logcum, precision=HIGHEST)
    cumulative = base_gate[:, None, :] + jnp.einsum(
        "sij,sjh->sih", ancestry, log_gates, precision=HIGHEST
    )
    gate_rows = jnp.swapaxes(cumulative, 1, 2)
    token_place = lax.axis_index("kv") * block_len + jnp.arange(block_len, dtype=jnp.int32)
    offset = token_place[None, :] - lengths[:, None]
    inserted = (offset >= 0) & (offset < accepted[:, None])
    one_hot = (offset[..., None] == jnp.arange(most_taken, dtype=jnp.int32)) & inserted[..., None]
    hot_low = one_hot.astype(jnp.bfloat16)
    merged_keys = jnp.where(
        inserted[..., None, None],
        jnp.einsum(
            "sla,sakd->slkd", hot_low, pending_keys, preferred_element_type=jnp.float32
        ).astype(jnp.bfloat16),
        cache_keys,
    )
    merged_values = jnp.where(
        inserted[..., None, None],
        jnp.einsum(
            "sla,sakd->slkd", hot_low, pending_values, preferred_element_type=jnp.float32
        ).astype(jnp.bfloat16),
        cache_values,
    )
    log_cache = jnp.where(
        inserted[..., None],
        jnp.einsum("sla,sah->slh", one_hot.astype(jnp.float32), pending_logcum, precision=HIGHEST),
        cache_logcum,
    )
    usable = token_place[None, :] < (lengths + accepted)[:, None]
    raw_scores = jnp.einsum(
        "spkgd,slkd->skgpl", queries, merged_keys, preferred_element_type=jnp.float32
    )
    scores = (
        raw_scores.reshape(seq_count, local_heads, node_count, block_len) * scaling
        + gate_rows[..., None]
        - jnp.swapaxes(log_cache, 1, 2)[:, :, None, :]
    )
    visible = usable[:, None, None, :]
    block_max = jnp.max(jnp.where(visible, scores, NEG_LARGE), axis=-1)
    weights = jnp.where(visible, jnp.exp(scores - block_max[..., None]), 0.0)
    block_sum = jnp.sum(weights, axis=-1)
    block_acc = jnp.einsum(
        "skgpl,slkd->skgpd",
        weights.astype(jnp.bfloat16).reshape(seq_count, key_heads, sharing, node_count, block_len),
        merged_values,
        preferred_element_type=jnp.float32,
    )
    block_acc = block_acc.reshape(seq_count, local_heads, node_count, head_size)
    tree_raw = jnp.einsum(
        "spkgd,sjkd->skgpj", queries, keys_new, preferred_element_type=jnp.float32
    )
    tree_scores = (
        tree_raw.reshape(seq_count, local_heads, node_count, node_count) * scaling
        + gate_rows[..., :, None]
        - gate_rows[..., None, :]
    )
    tree_mask = ancestry[:, None] > 0.5
    tree_max = jnp.max(jnp.where(tree_mask, tree_scores, NEG_LARGE), axis=-1)
    tree_weights = jnp.where(tree_mask, jnp.exp(tree_scores - tree_max[..., None]), 0.0)
    tree_sum = jnp.sum(tree_weights, axis=-1)
    tree_acc = jnp.einsum(
        "skgpj,sjkd->skgpd",
        tree_weights.astype(jnp.bfloat16).reshape(
            seq_count, key_heads, sharing, node_count, node_count
        ),
        values_new,
        preferred_element_type=jnp.float32,
    )
    tree_acc = tree_acc.reshape(seq_count, local_heads, node_count, head_size)
    tree_max_rows = to_rows(tree_max)
    tree_sum_rows = to_rows(tree_sum)
    tree_acc_rows = to_rows(tree_acc)
    cache_max, cache_sum, cache_acc = joined((block_max, block_sum, block_acc), "kv", join_blocks)
    attended = finish_rows(
        to_rows(cache_max),
        to_rows(cache_sum),
        to_rows(cache_acc),
        tree_max_rows,
        tree_sum_rows,
        tree_acc_rows,
    )
    head_part = jnp.dot(attended, output_weight, preferred_element_type=jnp.float32)
    head_part = head_part.reshape(seq_count, node_count, output_weight.shape[1])
    return lax.psum_scatter(head_part.astype(jnp.bfloat16), "tp", scatter_dimension=2, tiled=True)


LANES = 128
STAT_ROWS = 8
VMEM_LIMIT = 60 * 1024 * 1024
LARGE = 1e30
LOG2_E = 1.4426950408889634
TOKEN_PIECES = 4


def contract_last(left, right):
    return lax.dot_general(
        left, right, (((1,), (1,)), ((), ())), preferred_element_type=jnp.float32
    )


def plain_dot(left, right):
    return jnp.dot(left, right, preferred_element_type=jnp.float32)


def fused_kernel(ring, pair, pieces, names, order, *refs):
    inputs = dict(zip(names, refs))
    out_ref = refs[len(names)]
    held = dict(zip(names, refs[len(names) + 1 :]))
    (
        weight_buf,
        normed_buf,
        query_buf,
        part_buf,
        part_recv,
        stat_buf,
        stat_recv,
        att_buf,
        half_send,
        half_mine,
        half_recv,
        load_sem,
        token_sem,
        part_send_sem,
        part_recv_sem,
        stat_send_sem,
        stat_recv_sem,
        att_send_sem,
        att_recv_sem,
        half_send_sem,
        half_recv_sem,
    ) = refs[2 * len(names) + 1 - 3 :]
    me = lax.axis_index("kv")
    core = lax.axis_index("tp")
    partner = 1 - core
    tokens_buf, keys_buf, values_buf = held["tokens"], held["cache_keys"], held["cache_values"]
    seqs, heads, nodes, head_size = query_buf.shape
    rows, width = tokens_buf.shape
    block_len = keys_buf.shape[1]
    most_taken = held["pend_log"].shape[0]
    pend_rows = held["pend_keys"].shape[0]
    chunk = seqs // ring
    own_rows = chunk * nodes
    seq_rows = heads * nodes
    query_cols = heads * head_size
    half_cols = half_send.shape[2]
    seqs_per_tile = LANES // seq_rows
    tiles = chunk // seqs_per_tile
    tile_rows = seqs_per_tile * nodes
    scaling = head_size ** (-0.5)
    exponent = scaling * LOG2_E

    def target(step):
        low = jnp.where(ring - 1 - step > me, ring - 1 - step, ring - 2 - step)
        high = jnp.where(step < me, step, step + 1)
        return jnp.where(me < ring // 2, low, high)

    barrier = pltpu.get_barrier_semaphore()
    for step in range(ring - 1):
        pl.semaphore_signal(barrier, inc=1, device_id={"kv": lax.rem(me + step + 1, ring)})
    pl.semaphore_signal(barrier, inc=1, device_id={"tp": partner})

    places = dict(held)
    places["query_weight"] = weight_buf.at[:, 0:query_cols]
    places["key_weight"] = weight_buf.at[:, query_cols : query_cols + head_size]
    places["value_weight"] = weight_buf.at[:, query_cols + head_size : query_cols + 2 * head_size]
    piece_rows = rows // pieces
    token_loads = []
    for piece in range(pieces):
        span = pl.ds(piece * piece_rows, piece_rows)
        token_loads.append(
            pltpu.make_async_copy(
                inputs["tokens"].at[span], tokens_buf.at[span], token_sem.at[piece]
            )
        )
    loads = {
        name: pltpu.make_async_copy(inputs[name], places[name], load_sem.at[number])
        for number, name in enumerate(names)
        if name != "tokens"
    }
    loads["norm_gain"].start()
    for load in token_loads:
        load.start()
    loads["query_weight"].start()

    loads["norm_gain"].wait()
    gain = held["norm_gain"][...]
    step_rows = 16
    for piece in range(pieces):
        token_loads[piece].wait()
        if piece == 0:
            for name in order:
                if name not in ("tokens", "norm_gain", "query_weight"):
                    loads[name].start()

        def norm_rows(index, carry):
            place = pl.multiple_of(piece * piece_rows + index * step_rows, step_rows)
            span = pl.ds(place, step_rows)
            wide = tokens_buf[span, :].astype(jnp.float32)
            mean = jnp.sum(wide * wide, axis=-1, keepdims=True) * (1.0 / width)
            normed_buf[span, :] = (wide * lax.rsqrt(mean + EPSILON) * gain).astype(jnp.bfloat16)
            return carry

        lax.fori_loop(0, piece_rows // step_rows, norm_rows, 0, unroll=4)

    def head_scaled(vectors, gain_vec):
        mean = jnp.sum(vectors * vectors, axis=-1, keepdims=True) * (1.0 / head_size)
        return (vectors * lax.rsqrt(mean + EPSILON) * gain_vec).astype(jnp.bfloat16)

    loads["query_weight"].wait()
    loads["query_gain"].wait()
    for start in range(0, query_cols, 2 * head_size):
        part = plain_dot(normed_buf[...], weight_buf[:, start : start + 2 * head_size])
        for inner in range(2):
            vectors = part[:, inner * head_size : (inner + 1) * head_size]
            query_buf[:, start // head_size + inner] = head_scaled(
                vectors, held["query_gain"][...]
            ).reshape(seqs, nodes, head_size)

    for name in ("lengths", "cache_log", "cache_keys", "cache_values"):
        loads[name].wait()

    place = me * block_len + lax.broadcasted_iota(jnp.int32, (heads, block_len), 1)
    diagonal = lax.broadcasted_iota(jnp.int32, (LANES, LANES), 0) == lax.broadcasted_iota(
        jnp.int32, (LANES, LANES), 1
    )
    ones = jnp.ones((block_len, head_size), jnp.bfloat16)

    def spread_heads(table):
        return jnp.concatenate(
            [
                jnp.broadcast_to(table[head : head + 1, :], (nodes, table.shape[1]))
                for head in range(heads)
            ],
            axis=0,
        )

    def soft_part(scores, values, units):
        top = jnp.max(scores, axis=-1, keepdims=True)
        weights = jnp.exp2((scores - top) * exponent).astype(jnp.bfloat16)
        both = plain_dot(weights, jnp.concatenate([values, units], axis=1))
        total = both[:, head_size:]
        return both[:, :head_size] / total, top * scaling + jnp.log(total)

    def row_form(stats):
        column = jnp.concatenate(stats, axis=0)
        return jnp.sum(jnp.where(diagonal, column, 0.0), axis=0, keepdims=True)

    def stat_rows(stats):
        found = [
            row_form(stats[tile * seqs_per_tile : (tile + 1) * seqs_per_tile])
            for tile in range(tiles)
        ]
        return jnp.concatenate(
            found + [jnp.zeros((STAT_ROWS - tiles, LANES), jnp.float32)], axis=0
        )

    def attend(owner):
        values, stats = [], []
        for inner in range(chunk):
            seq = owner * chunk + inner
            query = query_buf[seq].reshape(seq_rows, head_size)
            bias = jnp.where(
                place < held["lengths"][seq], held["cache_log"][seq] * (1.0 / scaling), LARGE
            )
            scores = contract_last(query, keys_buf[seq]) - spread_heads(bias)
            value, stat = soft_part(scores, values_buf[seq], ones)
            values.append(value)
            stats.append(stat)
        return values, stats

    def send_part(step):
        there = target(step)
        return (
            pltpu.make_async_remote_copy(
                part_buf.at[step],
                part_recv.at[me],
                part_send_sem.at[step],
                part_recv_sem.at[me],
                device_id={"kv": there},
            ),
            pltpu.make_async_remote_copy(
                stat_buf.at[step],
                stat_recv.at[me],
                stat_send_sem.at[step],
                stat_recv_sem.at[me],
                device_id={"kv": there},
            ),
        )

    sends = []
    for step in range(ring - 1):
        values, stats = attend(target(step))
        for inner in range(chunk):
            part_buf[step, inner * seq_rows : (inner + 1) * seq_rows, :] = values[inner].astype(
                jnp.bfloat16
            )
        stat_buf[step] = stat_rows(stats)
        if step == 0:
            pl.semaphore_wait(barrier, ring)
        for copy in send_part(step):
            copy.start()
            sends.append(copy)

    own_values, own_stats = attend(me)
    own_stats = stat_rows(own_stats)

    for name in ("parents", "forget", "forget_bias", "accepted", "pend_log"):
        loads[name].wait()
    row_id = lax.broadcasted_iota(jnp.int32, (own_rows, seqs), 0)
    lane_id = lax.broadcasted_iota(jnp.int32, (own_rows, seqs), 1)
    spread = jnp.where(row_id // nodes + me * chunk == lane_id, 1.0, 0.0).astype(jnp.bfloat16)
    parent_rows = plain_dot(spread, held["parents"][...].astype(jnp.float32).astype(jnp.bfloat16))
    node_row = lax.broadcasted_iota(jnp.int32, (own_rows, nodes), 0)
    node_lane = lax.broadcasted_iota(jnp.int32, (own_rows, nodes), 1)
    parent = jnp.sum(
        jnp.where(node_row % nodes == node_lane, parent_rows, 0.0), axis=-1, keepdims=True
    )
    wide_row = lax.broadcasted_iota(jnp.int32, (own_rows, own_rows), 0)
    wide_lane = lax.broadcasted_iota(jnp.int32, (own_rows, own_rows), 1)
    lane_in_seq = (wide_lane - (wide_row // nodes) * nodes).astype(jnp.float32)
    linked = ((lane_in_seq == parent) & (parent >= 0.0)) | (wide_row == wide_lane)
    reach = jnp.where(linked, 1.0, 0.0).astype(jnp.bfloat16)
    for doubling in range((nodes - 1).bit_length()):
        reach = jnp.minimum(plain_dot(reach, reach), 1.0).astype(jnp.bfloat16)

    mine = pl.ds(pl.multiple_of(me * own_rows, own_rows), own_rows)
    own_normed = normed_buf[mine, :]
    all_heads = held["forget"].shape[0]
    square = (all_heads, all_heads)
    bias_column = jnp.sum(
        jnp.where(
            lax.broadcasted_iota(jnp.int32, square, 0) == lax.broadcasted_iota(jnp.int32, square, 1),
            jnp.broadcast_to(held["forget_bias"][...], square),
            0.0,
        ),
        axis=-1,
        keepdims=True,
    )
    logits = contract_last(held["forget"][...], own_normed) + bias_column
    log_gates = jnp.minimum(logits, 0.0) - jnp.log1p(jnp.exp(-jnp.abs(logits)))
    high = log_gates.astype(jnp.bfloat16)
    rest = log_gates - high.astype(jnp.float32)
    middle = rest.astype(jnp.bfloat16)
    low = (rest - middle.astype(jnp.float32)).astype(jnp.bfloat16)
    summed = contract_last(high, reach) + contract_last(middle, reach) + contract_last(low, reach)
    gates = summed[0:heads]
    for other in range(1, pair):
        gates = jnp.where(core == other, summed[other * heads : (other + 1) * heads], gates)

    for name in ("key_weight", "value_weight", "key_gain", "pend_keys", "pend_values"):
        loads[name].wait()
    part = plain_dot(own_normed, weight_buf[:, query_cols : query_cols + 2 * head_size])
    tree_keys = jnp.concatenate(
        [head_scaled(part[:, :head_size], held["key_gain"][...]), held["pend_keys"][...]], axis=0
    )
    tree_values = jnp.concatenate(
        [part[:, head_size:].astype(jnp.bfloat16), held["pend_values"][...]], axis=0
    )

    gate_head = lax.broadcasted_iota(jnp.int32, (heads, own_rows), 0)
    gate_seq = lax.broadcasted_iota(jnp.int32, (heads, own_rows), 1) // nodes
    pend_head = lax.broadcasted_iota(jnp.int32, (heads, pend_rows), 0)
    pend_lane = lax.broadcasted_iota(jnp.int32, (heads, pend_rows), 1)
    pend_bias = jnp.zeros((heads, pend_rows), jnp.float32)
    pend_seen = []
    pend_place = lax.broadcasted_iota(jnp.int32, (seq_rows, pend_rows), 1)
    for inner in range(chunk):
        seq = me * chunk + inner
        took = held["accepted"][seq]
        last_taken = jnp.maximum(took - 1, 0)
        first = seq * most_taken
        pend_seen.append((pend_place >= first) & (pend_place < first + took))
        for head in range(heads):
            base = held["pend_log"][last_taken, head, seq]
            gates = jnp.where((gate_head == head) & (gate_seq == inner), gates + base, gates)
            for number in range(most_taken):
                pend_bias = jnp.where(
                    (pend_head == head) & (pend_lane == first + number),
                    held["pend_log"][number, head, seq],
                    pend_bias,
                )
    tree_bias = spread_heads(
        jnp.concatenate([gates, pend_bias], axis=1) * (1.0 / scaling)
    )
    gate_stats = jnp.concatenate(
        [
            jnp.concatenate(
                [
                    gates[head : head + 1, inner * nodes : (inner + 1) * nodes]
                    for inner in range(tile * seqs_per_tile, (tile + 1) * seqs_per_tile)
                    for head in range(heads)
                ],
                axis=1,
            )
            for tile in range(tiles)
        ]
        + [jnp.zeros((STAT_ROWS - tiles, LANES), jnp.float32)],
        axis=0,
    )
    reached = reach.astype(jnp.float32)
    tree_ones = jnp.ones((own_rows + pend_rows, head_size), jnp.bfloat16)
    tree_parts, tree_stats = [], []
    for inner in range(chunk):
        query = query_buf[me * chunk + inner].reshape(seq_rows, head_size)
        seen = jnp.concatenate(
            [
                jnp.concatenate([reached[inner * nodes : (inner + 1) * nodes, :]] * heads, axis=0),
                jnp.where(pend_seen[inner], 1.0, 0.0),
            ],
            axis=1,
        )
        scores = contract_last(query, tree_keys) - jnp.where(seen > 0.5, tree_bias, LARGE)
        value, stat = soft_part(scores, tree_values, tree_ones)
        tree_parts.append(value)
        tree_stats.append(stat)
    tree_stats = stat_rows(tree_stats)

    for step in range(ring - 1):
        source = target(step)
        for buffer, received, send_sems, recv_sems in (
            (part_buf, part_recv, part_send_sem, part_recv_sem),
            (stat_buf, stat_recv, stat_send_sem, stat_recv_sem),
        ):
            pltpu.make_async_remote_copy(
                buffer.at[step],
                received.at[source],
                send_sems.at[step],
                recv_sems.at[source],
                device_id={"kv": source},
            ).wait_recv()
    stats = [tree_stats, own_stats] + [
        stat_recv[target(step)] for step in range(ring - 1)
    ]
    stats = [stat + gate_stats for stat in stats]
    top = functools.reduce(jnp.maximum, stats)
    factors = [jnp.exp(stat - top) for stat in stats]
    whole = functools.reduce(jnp.add, factors)
    factors = [factor / whole for factor in factors]
    blank = jnp.zeros((LANES - STAT_ROWS * len(factors), LANES), jnp.float32)
    factor_cols = jnp.concatenate(factors + [blank], axis=0).T
    for inner in range(chunk):
        tile = inner // seqs_per_tile
        lanes = slice((inner % seqs_per_tile) * seq_rows, (inner % seqs_per_tile + 1) * seq_rows)
        span = slice(inner * seq_rows, (inner + 1) * seq_rows)
        sources = [tree_parts[inner], own_values[inner]] + [
            part_recv[target(step), span, :].astype(jnp.float32) for step in range(ring - 1)
        ]
        mixed = None
        for number, source in enumerate(sources):
            lane = number * STAT_ROWS + tile
            term = factor_cols[lanes, lane : lane + 1] * source
            mixed = term if mixed is None else mixed + term
        mixed = mixed.astype(jnp.bfloat16)
        for head in range(heads):
            att_buf[
                me,
                inner * nodes : (inner + 1) * nodes,
                head * head_size : (head + 1) * head_size,
            ] = mixed[head * nodes : (head + 1) * nodes, :]
    att_sends = []
    for step in range(ring - 1):
        copy = pltpu.make_async_remote_copy(
            att_buf.at[me],
            att_buf.at[me],
            att_send_sem.at[step],
            att_recv_sem.at[me],
            device_id={"kv": target(step)},
        )
        copy.start()
        att_sends.append(copy)

    loads["output_weight"].wait()
    theirs = pl.ds(pl.multiple_of(partner * half_cols, LANES), half_cols)
    ours = pl.ds(pl.multiple_of(core * half_cols, LANES), half_cols)
    output_weight_buf = held["output_weight"]
    half_sends = []
    for spot in range(ring):
        origin = me if spot == 0 else target(ring - 1 - spot)
        if spot > 0:
            pltpu.make_async_remote_copy(
                att_buf.at[origin],
                att_buf.at[origin],
                att_send_sem.at[spot - 1],
                att_recv_sem.at[origin],
                device_id={"kv": origin},
            ).wait_recv()
        attended = att_buf[origin]
        half_send[spot] = plain_dot(attended, output_weight_buf[:, theirs]).astype(jnp.bfloat16)
        copy = pltpu.make_async_remote_copy(
            half_send.at[spot],
            half_recv.at[spot],
            half_send_sem.at[spot],
            half_recv_sem.at[spot],
            device_id={"tp": partner},
        )
        copy.start()
        half_sends.append(copy)
        half_mine[spot] = plain_dot(attended, output_weight_buf[:, ours]).astype(jnp.bfloat16)
    for spot in range(ring):
        origin = me if spot == 0 else target(ring - 1 - spot)
        half_sends[spot].wait_recv()
        out_ref[origin] = (
            half_mine[spot].astype(jnp.float32) + half_recv[spot].astype(jnp.float32)
        ).astype(jnp.bfloat16)
    for copy in sends + att_sends + half_sends:
        copy.wait_send()


def fused(
    ring,
    pair,
    tokens,
    norm_gain,
    query_weight,
    key_weight,
    value_weight,
    forget_weight,
    forget_bias,
    query_gain,
    key_gain,
    output_weight,
    cache_keys,
    cache_values,
    cache_logcum,
    pending_keys,
    pending_values,
    pending_logcum,
    lengths,
    accepted,
    parents,
):
    seqs, nodes, width = tokens.shape
    head_size = query_gain.shape[0]
    query_cols = query_weight.shape[1]
    heads = query_cols // head_size
    block_len = cache_keys.shape[1]
    rows = seqs * nodes
    half_cols = output_weight.shape[1] // pair
    chunk = seqs // ring
    chunk_rows = chunk * nodes
    part_rows = chunk_rows * heads
    pieces = TOKEN_PIECES if rows % (64 * TOKEN_PIECES) == 0 else 1
    arrays = {
        "tokens": tokens.reshape(rows, width),
        "norm_gain": norm_gain.reshape(1, width),
        "query_weight": query_weight,
        "query_gain": query_gain.reshape(1, head_size),
        "lengths": lengths,
        "cache_log": jnp.swapaxes(cache_logcum, 1, 2),
        "cache_keys": cache_keys.reshape(seqs, block_len, head_size),
        "cache_values": cache_values.reshape(seqs, block_len, head_size),
        "parents": parents,
        "forget": forget_weight.T,
        "forget_bias": forget_bias.reshape(1, -1),
        "accepted": accepted,
        "pend_log": jnp.transpose(pending_logcum, (1, 2, 0)),
        "key_weight": key_weight,
        "value_weight": value_weight,
        "key_gain": key_gain.reshape(1, head_size),
        "pend_keys": pending_keys.reshape(-1, head_size),
        "pend_values": pending_values.reshape(-1, head_size),
        "output_weight": output_weight,
    }
    scalars = ("lengths", "accepted", "pend_log")
    joined_loads = ("query_weight", "key_weight", "value_weight")
    names = tuple(name for name in arrays if name not in joined_loads) + joined_loads
    order = tuple(arrays)
    held = [
        (pltpu.SMEM if name in scalars else pltpu.VMEM)(arrays[name].shape, arrays[name].dtype)
        for name in names
        if name not in joined_loads
    ]
    low, wide = jnp.bfloat16, jnp.float32
    sems = pltpu.SemaphoreType.DMA
    result = pl.pallas_call(
        functools.partial(fused_kernel, ring, pair, pieces, names, order),
        out_shape=pltpu.VMEM((ring, chunk_rows, half_cols), low),
        in_specs=[pl.BlockSpec(memory_space=pltpu.HBM)] * len(names),
        out_specs=pl.BlockSpec(memory_space=pltpu.VMEM),
        scratch_shapes=held
        + [
            pltpu.VMEM((width, query_cols + 2 * head_size), low),
            pltpu.VMEM((rows, width), low),
            pltpu.VMEM((seqs, heads, nodes, head_size), low),
            pltpu.VMEM((ring - 1, part_rows, head_size), low),
            pltpu.VMEM((ring, part_rows, head_size), low),
            pltpu.VMEM((ring - 1, STAT_ROWS, LANES), wide),
            pltpu.VMEM((ring, STAT_ROWS, LANES), wide),
            pltpu.VMEM((ring, chunk_rows, query_cols), low),
            pltpu.VMEM((ring, chunk_rows, half_cols), low),
            pltpu.VMEM((ring, chunk_rows, half_cols), low),
            pltpu.VMEM((ring, chunk_rows, half_cols), low),
            sems((len(names),)),
            sems((pieces,)),
            sems((ring - 1,)),
            sems((ring,)),
            sems((ring - 1,)),
            sems((ring,)),
            sems((ring - 1,)),
            sems((ring,)),
            sems((ring,)),
            sems((ring,)),
        ],
        compiler_params=pltpu.CompilerParams(
            collective_id=0, has_side_effects=True, vmem_limit_bytes=VMEM_LIMIT
        ),
    )(*[arrays[name] for name in names])
    return result.reshape(seqs, nodes, half_cols)


def layer(ring, pair, *arrays):
    tokens, output_weight, cache_keys = arrays[0], arrays[9], arrays[10]
    seqs, nodes = tokens.shape[:2]
    head_size = arrays[7].shape[0]
    heads = arrays[2].shape[1] // head_size
    fits = (
        ring > 1
        and pair == 2
        and head_size == LANES
        and cache_keys.shape[2] == 1
        and cache_keys.shape[1] % LANES == 0
        and nodes % 16 == 0
        and LANES % (heads * nodes) == 0
        and heads % 2 == 0
        and seqs % ring == 0
        and (seqs // ring * heads * nodes) % LANES == 0
        and STAT_ROWS * (ring + 1) <= LANES
        and seqs // ring * heads * nodes // LANES <= STAT_ROWS
        and seqs // ring * nodes + seqs * arrays[13].shape[1] == LANES
        and (seqs * nodes) % LANES == 0
        and output_weight.shape[1] % (pair * LANES) == 0
    )
    if fits:
        return fused(ring, pair, *arrays)
    return shards(*arrays)


def solution(mesh):
    placed = (
        P("dp", None, None),
        P(),
        P(None, "tp"),
        P(None, "tp"),
        P(None, "tp"),
        P(),
        P(),
        P(),
        P(),
        P("tp", "kv"),
        P("dp", "kv", "tp", None),
        P("dp", "kv", "tp", None),
        P("dp", "kv", "tp"),
        P("dp", None, "tp", None),
        P("dp", None, "tp", None),
        P("dp", None, "tp"),
        P("dp"),
        P("dp"),
        P("dp", None),
    )
    return jax.shard_map(
        functools.partial(layer, mesh.shape["kv"], mesh.shape["tp"]), mesh=mesh, in_specs=placed, out_specs=P("dp", None, ("kv", "tp")), check_vma=False
    )
```

```python
import functools

import jax
import jax.numpy as jnp
from jax import lax
from jax.experimental import pallas as pl
from jax.experimental.pallas import tpu as pltpu
from jax.sharding import PartitionSpec as P

EPSILON = 1e-06
NEG_LARGE = -1e30
HIGHEST = lax.Precision.HIGHEST


def joined(shard, axis, join):
    gathered = jax.tree.map(
        lambda a, kind: lax.all_gather(a.astype(kind), axis),
        shard,
        (jnp.bfloat16, jnp.bfloat16, jnp.bfloat16),
    )

    def take(source):
        return jax.tree.map(
            lambda a, own: lax.dynamic_index_in_dim(a, source, 0, False).astype(own.dtype),
            gathered,
            shard,
        )

    return lax.fori_loop(
        1, lax.axis_size(axis), lambda source, state: join(state, take(source)), take(0)
    )


def head_norm(vectors, gain_vec):
    return (
        vectors
        * lax.rsqrt(jnp.mean(vectors * vectors, axis=-1, keepdims=True) + EPSILON)
        * gain_vec
    )


def ancestors(parents):
    node_count = parents.shape[-1]
    indices = jnp.arange(node_count, dtype=jnp.int32)
    reachable = (parents[..., None] == indices).astype(jnp.float32) + jnp.eye(
        node_count, dtype=jnp.float32
    )
    for doubling in range((node_count - 1).bit_length()):
        reachable = jnp.minimum(
            jnp.einsum("sij,sjk->sik", reachable, reachable, precision=HIGHEST), 1.0
        )
    return reachable


def join_blocks(earlier, later):
    larger = jnp.maximum(earlier[0], later[0])
    left_factor = jnp.exp(earlier[0] - larger)
    right_factor = jnp.exp(later[0] - larger)
    return (
        larger,
        earlier[1] * left_factor + later[1] * right_factor,
        earlier[2] * left_factor[..., None] + later[2] * right_factor[..., None],
    )


def to_rows(values):
    moved = jnp.swapaxes(values, 1, 2)
    return moved.reshape((moved.shape[0] * moved.shape[1],) + moved.shape[2:])


def finish_rows(cache_max, cache_sum, cache_acc, tree_max, tree_sum, tree_acc):
    overall = jnp.maximum(cache_max, tree_max)
    factor_cache = jnp.exp(cache_max - overall)
    factor_tree = jnp.exp(tree_max - overall)
    denominator = cache_sum * factor_cache + tree_sum * factor_tree
    numerator = cache_acc * factor_cache[..., None] + tree_acc * factor_tree[..., None]
    attended = (numerator / denominator[..., None]).astype(jnp.bfloat16)
    return attended.reshape(attended.shape[0], attended.shape[1] * attended.shape[2])


def shards(
    tokens,
    norm_gain,
    query_weight,
    key_weight,
    value_weight,
    forget_weight,
    forget_bias,
    query_gain,
    key_gain,
    output_weight,
    cache_keys,
    cache_values,
    cache_logcum,
    pending_keys,
    pending_values,
    pending_logcum,
    lengths,
    accepted,
    parents,
):
    seq_count, node_count, model_width = tokens.shape
    token_rows = seq_count * node_count
    head_size = query_gain.shape[0]
    query_cols = query_weight.shape[1]
    key_cols = key_weight.shape[1]
    local_heads = query_cols // head_size
    key_heads = key_cols // head_size
    sharing = local_heads // key_heads
    block_len = cache_keys.shape[1]
    most_taken = pending_keys.shape[1]
    scaling = head_size ** (-0.5)
    widened = tokens.reshape(token_rows, model_width).astype(jnp.float32)
    normed = (
        widened
        * lax.rsqrt(jnp.mean(widened * widened, axis=-1, keepdims=True) + EPSILON)
        * norm_gain
    ).astype(jnp.bfloat16)
    joined_weight = jnp.concatenate([query_weight, key_weight, value_weight], axis=1)
    summed = jnp.dot(normed, joined_weight, preferred_element_type=jnp.float32)
    query_part = head_norm(
        summed[:, :query_cols].reshape(token_rows, local_heads, head_size), query_gain
    )
    key_part = head_norm(
        summed[:, query_cols : query_cols + key_cols].reshape(token_rows, key_heads, head_size),
        key_gain,
    )
    queries = query_part.astype(jnp.bfloat16).reshape(
        seq_count, node_count, key_heads, sharing, head_size
    )
    keys_new = key_part.astype(jnp.bfloat16).reshape(seq_count, node_count, key_heads, head_size)
    values_new = (
        summed[:, query_cols + key_cols :]
        .astype(jnp.bfloat16)
        .reshape(seq_count, node_count, key_heads, head_size)
    )
    head_start = lax.axis_index("tp") * local_heads
    forget_cols = lax.dynamic_slice_in_dim(forget_weight, head_start, local_heads, 1)
    gate_bias = lax.dynamic_slice_in_dim(forget_bias, head_start, local_heads, 0)
    log_gates = jax.nn.log_sigmoid(
        jnp.dot(normed, forget_cols, preferred_element_type=jnp.float32) + gate_bias
    ).reshape(seq_count, node_count, local_heads)
    ancestry = ancestors(parents)
    choose = (jnp.arange(most_taken, dtype=jnp.int32)[None, :] == (accepted - 1)[:, None]).astype(
        jnp.float32
    )
    base_gate = jnp.einsum("sa,sah->sh", choose, pending_logcum, precision=HIGHEST)
    cumulative = base_gate[:, None, :] + jnp.einsum(
        "sij,sjh->sih", ancestry, log_gates, precision=HIGHEST
    )
    gate_rows = jnp.swapaxes(cumulative, 1, 2)
    token_place = lax.axis_index("kv") * block_len + jnp.arange(block_len, dtype=jnp.int32)
    offset = token_place[None, :] - lengths[:, None]
    inserted = (offset >= 0) & (offset < accepted[:, None])
    one_hot = (offset[..., None] == jnp.arange(most_taken, dtype=jnp.int32)) & inserted[..., None]
    hot_low = one_hot.astype(jnp.bfloat16)
    merged_keys = jnp.where(
        inserted[..., None, None],
        jnp.einsum(
            "sla,sakd->slkd", hot_low, pending_keys, preferred_element_type=jnp.float32
        ).astype(jnp.bfloat16),
        cache_keys,
    )
    merged_values = jnp.where(
        inserted[..., None, None],
        jnp.einsum(
            "sla,sakd->slkd", hot_low, pending_values, preferred_element_type=jnp.float32
        ).astype(jnp.bfloat16),
        cache_values,
    )
    log_cache = jnp.where(
        inserted[..., None],
        jnp.einsum("sla,sah->slh", one_hot.astype(jnp.float32), pending_logcum, precision=HIGHEST),
        cache_logcum,
    )
    usable = token_place[None, :] < (lengths + accepted)[:, None]
    raw_scores = jnp.einsum(
        "spkgd,slkd->skgpl", queries, merged_keys, preferred_element_type=jnp.float32
    )
    scores = (
        raw_scores.reshape(seq_count, local_heads, node_count, block_len) * scaling
        + gate_rows[..., None]
        - jnp.swapaxes(log_cache, 1, 2)[:, :, None, :]
    )
    visible = usable[:, None, None, :]
    block_max = jnp.max(jnp.where(visible, scores, NEG_LARGE), axis=-1)
    weights = jnp.where(visible, jnp.exp(scores - block_max[..., None]), 0.0)
    block_sum = jnp.sum(weights, axis=-1)
    block_acc = jnp.einsum(
        "skgpl,slkd->skgpd",
        weights.astype(jnp.bfloat16).reshape(seq_count, key_heads, sharing, node_count, block_len),
        merged_values,
        preferred_element_type=jnp.float32,
    )
    block_acc = block_acc.reshape(seq_count, local_heads, node_count, head_size)
    tree_raw = jnp.einsum(
        "spkgd,sjkd->skgpj", queries, keys_new, preferred_element_type=jnp.float32
    )
    tree_scores = (
        tree_raw.reshape(seq_count, local_heads, node_count, node_count) * scaling
        + gate_rows[..., :, None]
        - gate_rows[..., None, :]
    )
    tree_mask = ancestry[:, None] > 0.5
    tree_max = jnp.max(jnp.where(tree_mask, tree_scores, NEG_LARGE), axis=-1)
    tree_weights = jnp.where(tree_mask, jnp.exp(tree_scores - tree_max[..., None]), 0.0)
    tree_sum = jnp.sum(tree_weights, axis=-1)
    tree_acc = jnp.einsum(
        "skgpj,sjkd->skgpd",
        tree_weights.astype(jnp.bfloat16).reshape(
            seq_count, key_heads, sharing, node_count, node_count
        ),
        values_new,
        preferred_element_type=jnp.float32,
    )
    tree_acc = tree_acc.reshape(seq_count, local_heads, node_count, head_size)
    tree_max_rows = to_rows(tree_max)
    tree_sum_rows = to_rows(tree_sum)
    tree_acc_rows = to_rows(tree_acc)
    cache_max, cache_sum, cache_acc = joined((block_max, block_sum, block_acc), "kv", join_blocks)
    attended = finish_rows(
        to_rows(cache_max),
        to_rows(cache_sum),
        to_rows(cache_acc),
        tree_max_rows,
        tree_sum_rows,
        tree_acc_rows,
    )
    head_part = jnp.dot(attended, output_weight, preferred_element_type=jnp.float32)
    head_part = head_part.reshape(seq_count, node_count, output_weight.shape[1])
    return lax.psum_scatter(head_part.astype(jnp.bfloat16), "tp", scatter_dimension=2, tiled=True)


LANES = 128
STAT_ROWS = 8
STAT_PARTS = 3
VMEM_LIMIT = 60 * 1024 * 1024
LARGE = 1e30
LOG2_E = 1.4426950408889634
TOKEN_PIECES = 4


def contract_last(left, right):
    return lax.dot_general(
        left, right, (((1,), (1,)), ((), ())), preferred_element_type=jnp.float32
    )


def plain_dot(left, right):
    return jnp.dot(left, right, preferred_element_type=jnp.float32)


def fused_kernel(ring, pair, pieces, names, order, *refs):
    inputs = dict(zip(names, refs))
    out_ref = refs[len(names)]
    held = dict(zip(names, refs[len(names) + 1 :]))
    (
        weight_buf,
        normed_buf,
        query_buf,
        part_buf,
        part_recv,
        full_weight,
        att_buf,
        half_send,
        half_recv,
        load_sem,
        token_sem,
        part_send_sem,
        part_recv_sem,
        att_send_sem,
        att_recv_sem,
        half_send_sem,
        half_recv_sem,
        local_send_sem,
        weight_sems,
    ) = refs[2 * len(names) + 1 - 4 :]
    me = lax.axis_index("kv")
    core = lax.axis_index("tp")
    partner = 1 - core
    last = pair - 1
    tokens_buf, keys_buf, values_buf = held["tokens"], held["cache_keys"], held["cache_values"]
    seqs, heads, nodes, head_size = query_buf.shape
    rows, width = tokens_buf.shape
    block_len = keys_buf.shape[1]
    most_taken = held["pend_log"].shape[0]
    pend_rows = held["pend_keys"].shape[0]
    chunk = seqs // ring
    own_rows = chunk * nodes
    seq_rows = heads * nodes
    query_cols = heads * head_size
    half_cols = half_send.shape[2]
    seqs_per_tile = LANES // seq_rows
    tiles = chunk // seqs_per_tile
    tile_rows = seqs_per_tile * nodes
    part_rows = chunk * seq_rows
    scaling = head_size ** (-0.5)
    exponent = scaling * LOG2_E

    def target(step):
        step = ring - 2 - step
        low = jnp.where(ring - 1 - step > me, ring - 1 - step, ring - 2 - step)
        high = jnp.where(step < me, step, step + 1)
        return jnp.where(me < ring // 2, low, high)

    barrier = pltpu.get_barrier_semaphore()
    for step in range(ring - 1):
        for other in range(pair):
            pl.semaphore_signal(
                barrier, inc=1, device_id={"kv": lax.rem(me + step + 1, ring), "tp": other}
            )
    pl.semaphore_signal(barrier, inc=1, device_id={"tp": partner})

    places = dict(held)
    places["query_weight"] = weight_buf.at[:, 0:query_cols]
    places["output_weight"] = full_weight.at[core]
    places["key_weight"] = weight_buf.at[:, query_cols : query_cols + head_size]
    places["value_weight"] = weight_buf.at[:, query_cols + head_size : query_cols + 2 * head_size]
    piece_rows = rows // pieces
    token_loads = []
    for piece in range(pieces):
        span = pl.ds(piece * piece_rows, piece_rows)
        token_loads.append(
            pltpu.make_async_copy(
                inputs["tokens"].at[span], tokens_buf.at[span], token_sem.at[piece]
            )
        )
    loads = {
        name: pltpu.make_async_copy(inputs[name], places[name], load_sem.at[number])
        for number, name in enumerate(names)
        if name != "tokens"
    }
    loads["norm_gain"].start()
    for load in token_loads:
        load.start()
    loads["query_weight"].start()

    loads["norm_gain"].wait()
    gain = held["norm_gain"][...]
    step_rows = 16
    for piece in range(pieces):
        token_loads[piece].wait()
        if piece == 0:
            for name in order:
                if name not in ("tokens", "norm_gain", "query_weight"):
                    loads[name].start()

        def norm_rows(index, carry):
            place = pl.multiple_of(piece * piece_rows + index * step_rows, step_rows)
            span = pl.ds(place, step_rows)
            wide = tokens_buf[span, :].astype(jnp.float32)
            mean = jnp.sum(wide * wide, axis=-1, keepdims=True) * (1.0 / width)
            normed_buf[span, :] = (wide * lax.rsqrt(mean + EPSILON) * gain).astype(jnp.bfloat16)
            return carry

        lax.fori_loop(0, piece_rows // step_rows, norm_rows, 0, unroll=4)

    def head_scaled(vectors, gain_vec):
        mean = jnp.sum(vectors * vectors, axis=-1, keepdims=True) * (1.0 / head_size)
        return (vectors * lax.rsqrt(mean + EPSILON) * gain_vec).astype(jnp.bfloat16)

    loads["query_weight"].wait()
    loads["query_gain"].wait()
    for start in range(0, query_cols, 2 * head_size):
        part = plain_dot(normed_buf[...], weight_buf[:, start : start + 2 * head_size])
        for inner in range(2):
            vectors = part[:, inner * head_size : (inner + 1) * head_size]
            query_buf[:, start // head_size + inner] = head_scaled(
                vectors, held["query_gain"][...]
            ).reshape(seqs, nodes, head_size)

    for name in ("lengths", "cache_log", "cache_keys", "cache_values"):
        loads[name].wait()

    place = me * block_len + lax.broadcasted_iota(jnp.int32, (heads, block_len), 1)
    diagonal = lax.broadcasted_iota(jnp.int32, (LANES, LANES), 0) == lax.broadcasted_iota(
        jnp.int32, (LANES, LANES), 1
    )
    ones = jnp.ones((block_len, head_size), jnp.bfloat16)

    def spread_heads(table):
        return jnp.concatenate(
            [
                jnp.broadcast_to(table[head : head + 1, :], (nodes, table.shape[1]))
                for head in range(heads)
            ],
            axis=0,
        )

    def soft_part(scores, values, units):
        top = jnp.max(scores, axis=-1, keepdims=True)
        weights = jnp.exp2((scores - top) * exponent).astype(jnp.bfloat16)
        both = plain_dot(weights, jnp.concatenate([values, units], axis=1))
        total = both[:, head_size:]
        return both[:, :head_size] / total, top * scaling + jnp.log(total)

    def row_form(stats):
        column = jnp.concatenate(stats, axis=0)
        return jnp.sum(jnp.where(diagonal, column, 0.0), axis=0, keepdims=True)

    def stat_rows(stats):
        found = [
            row_form(stats[tile * seqs_per_tile : (tile + 1) * seqs_per_tile])
            for tile in range(tiles)
        ]
        return jnp.concatenate(
            found + [jnp.zeros((STAT_ROWS - tiles, LANES), jnp.float32)], axis=0
        )

    def attend(owner):
        values, stats = [], []
        for inner in range(chunk):
            seq = owner * chunk + inner
            query = query_buf[seq].reshape(seq_rows, head_size)
            bias = jnp.where(
                place < held["lengths"][seq], held["cache_log"][seq] * (1.0 / scaling), LARGE
            )
            scores = contract_last(query, keys_buf[seq]) - spread_heads(bias)
            value, stat = soft_part(scores, values_buf[seq], ones)
            values.append(value)
            stats.append(stat)
        return values, stats

    def pack(stats):
        rest = stats[0:tiles]
        found = []
        for number in range(STAT_PARTS):
            found.append(rest.astype(jnp.bfloat16).astype(jnp.float32))
            rest = rest - found[-1]
        blank = jnp.zeros((2 * STAT_ROWS - STAT_PARTS * tiles, LANES), jnp.float32)
        return jnp.concatenate(found + [blank], axis=0).astype(jnp.bfloat16)

    def unpack(source):
        packed = part_recv[source, part_rows : part_rows + 2 * STAT_ROWS, :].astype(jnp.float32)
        return jnp.concatenate(
            [
                functools.reduce(
                    jnp.add,
                    [
                        packed[number * tiles : (number + 1) * tiles]
                        for number in range(STAT_PARTS)
                    ],
                ),
                jnp.zeros((STAT_ROWS - tiles, LANES), jnp.float32),
            ],
            axis=0,
        )

    def send_part(step, there):
        return pltpu.make_async_remote_copy(
            part_buf.at[step],
            part_recv.at[me],
            part_send_sem.at[step],
            part_recv_sem.at[me],
            device_id={"kv": there},
        )

    sends = []
    for step in range(ring - 1):
        there = target(ring - 2 - step)
        values, stats = attend(there)
        for inner in range(chunk):
            part_buf[step, inner * seq_rows : (inner + 1) * seq_rows, :] = values[inner].astype(
                jnp.bfloat16
            )
        part_buf[step, part_rows : part_rows + 2 * STAT_ROWS, :] = pack(stat_rows(stats))
        if step == 0:
            pl.semaphore_wait(barrier, (ring - 1) * pair + 1)
        copy = send_part(step, there)
        copy.start()
        sends.append(copy)

    own_values, own_stats = attend(me)
    own_stats = stat_rows(own_stats)

    for name in ("parents", "forget", "forget_bias", "accepted", "pend_log"):
        loads[name].wait()
    row_id = lax.broadcasted_iota(jnp.int32, (own_rows, seqs), 0)
    lane_id = lax.broadcasted_iota(jnp.int32, (own_rows, seqs), 1)
    spread = jnp.where(row_id // nodes + me * chunk == lane_id, 1.0, 0.0).astype(jnp.bfloat16)
    parent_rows = plain_dot(spread, held["parents"][...].astype(jnp.float32).astype(jnp.bfloat16))
    node_row = lax.broadcasted_iota(jnp.int32, (own_rows, nodes), 0)
    node_lane = lax.broadcasted_iota(jnp.int32, (own_rows, nodes), 1)
    parent = jnp.sum(
        jnp.where(node_row % nodes == node_lane, parent_rows, 0.0), axis=-1, keepdims=True
    )
    wide_row = lax.broadcasted_iota(jnp.int32, (own_rows, own_rows), 0)
    wide_lane = lax.broadcasted_iota(jnp.int32, (own_rows, own_rows), 1)
    lane_in_seq = (wide_lane - (wide_row // nodes) * nodes).astype(jnp.float32)
    linked = ((lane_in_seq == parent) & (parent >= 0.0)) | (wide_row == wide_lane)
    reach = jnp.where(linked, 1.0, 0.0).astype(jnp.bfloat16)
    for doubling in range((nodes - 1).bit_length()):
        reach = jnp.minimum(plain_dot(reach, reach), 1.0).astype(jnp.bfloat16)

    mine = pl.ds(pl.multiple_of(me * own_rows, own_rows), own_rows)
    own_normed = normed_buf[mine, :]
    all_heads = held["forget"].shape[0]
    square = (all_heads, all_heads)
    bias_column = jnp.sum(
        jnp.where(
            lax.broadcasted_iota(jnp.int32, square, 0) == lax.broadcasted_iota(jnp.int32, square, 1),
            jnp.broadcast_to(held["forget_bias"][...], square),
            0.0,
        ),
        axis=-1,
        keepdims=True,
    )
    logits = contract_last(held["forget"][...], own_normed) + bias_column
    log_gates = jnp.minimum(logits, 0.0) - jnp.log1p(jnp.exp(-jnp.abs(logits)))
    high = log_gates.astype(jnp.bfloat16)
    rest = log_gates - high.astype(jnp.float32)
    middle = rest.astype(jnp.bfloat16)
    low = (rest - middle.astype(jnp.float32)).astype(jnp.bfloat16)
    summed = contract_last(high, reach) + contract_last(middle, reach) + contract_last(low, reach)
    gates = summed[0:heads]
    for other in range(1, pair):
        gates = jnp.where(core == other, summed[other * heads : (other + 1) * heads], gates)

    for name in ("key_weight", "value_weight", "key_gain", "pend_keys", "pend_values"):
        loads[name].wait()
    part = plain_dot(own_normed, weight_buf[:, query_cols : query_cols + 2 * head_size])
    tree_keys = jnp.concatenate(
        [head_scaled(part[:, :head_size], held["key_gain"][...]), held["pend_keys"][...]], axis=0
    )
    tree_values = jnp.concatenate(
        [part[:, head_size:].astype(jnp.bfloat16), held["pend_values"][...]], axis=0
    )

    gate_head = lax.broadcasted_iota(jnp.int32, (heads, own_rows), 0)
    gate_seq = lax.broadcasted_iota(jnp.int32, (heads, own_rows), 1) // nodes
    pend_head = lax.broadcasted_iota(jnp.int32, (heads, pend_rows), 0)
    pend_lane = lax.broadcasted_iota(jnp.int32, (heads, pend_rows), 1)
    pend_bias = jnp.zeros((heads, pend_rows), jnp.float32)
    pend_seen = []
    pend_place = lax.broadcasted_iota(jnp.int32, (seq_rows, pend_rows), 1)
    for inner in range(chunk):
        seq = me * chunk + inner
        took = held["accepted"][seq]
        last_taken = jnp.maximum(took - 1, 0)
        first = seq * most_taken
        pend_seen.append((pend_place >= first) & (pend_place < first + took))
        for head in range(heads):
            base = held["pend_log"][last_taken, head, seq]
            gates = jnp.where((gate_head == head) & (gate_seq == inner), gates + base, gates)
            for number in range(most_taken):
                pend_bias = jnp.where(
                    (pend_head == head) & (pend_lane == first + number),
                    held["pend_log"][number, head, seq],
                    pend_bias,
                )
    tree_bias = spread_heads(
        jnp.concatenate([gates, pend_bias], axis=1) * (1.0 / scaling)
    )
    gate_stats = jnp.concatenate(
        [
            jnp.concatenate(
                [
                    gates[head : head + 1, inner * nodes : (inner + 1) * nodes]
                    for inner in range(tile * seqs_per_tile, (tile + 1) * seqs_per_tile)
                    for head in range(heads)
                ],
                axis=1,
            )
            for tile in range(tiles)
        ]
        + [jnp.zeros((STAT_ROWS - tiles, LANES), jnp.float32)],
        axis=0,
    )
    reached = reach.astype(jnp.float32)
    tree_ones = jnp.ones((own_rows + pend_rows, head_size), jnp.bfloat16)
    tree_parts, tree_stats = [], []
    for inner in range(chunk):
        query = query_buf[me * chunk + inner].reshape(seq_rows, head_size)
        seen = jnp.concatenate(
            [
                jnp.concatenate([reached[inner * nodes : (inner + 1) * nodes, :]] * heads, axis=0),
                jnp.where(pend_seen[inner], 1.0, 0.0),
            ],
            axis=1,
        )
        scores = contract_last(query, tree_keys) - jnp.where(seen > 0.5, tree_bias, LARGE)
        value, stat = soft_part(scores, tree_values, tree_ones)
        tree_parts.append(value)
        tree_stats.append(stat)
    tree_stats = stat_rows(tree_stats)

    def weigh(stats):
        top = functools.reduce(jnp.maximum, stats)
        factors = [jnp.exp(stat - top) for stat in stats]
        whole = functools.reduce(jnp.add, factors)
        factors = [factor / whole for factor in factors]
        blank = jnp.zeros((LANES - STAT_ROWS * len(factors), LANES), jnp.float32)
        return jnp.concatenate(factors + [blank], axis=0).T, top + jnp.log(whole)

    def mix(columns, inner, sources):
        tile = inner // seqs_per_tile
        first = (inner % seqs_per_tile) * seq_rows
        mixed = None
        for number, source in enumerate(sources):
            lane = number * STAT_ROWS + tile
            term = columns[first : first + seq_rows, lane : lane + 1] * source
            mixed = term if mixed is None else mixed + term
        return mixed

    columns, local_stats = weigh([tree_stats + gate_stats, own_stats + gate_stats])
    local_parts = [
        mix(columns, inner, [tree_parts[inner], own_values[inner]]) for inner in range(chunk)
    ]

    loads["output_weight"].wait()
    weight_push = pltpu.make_async_remote_copy(
        full_weight.at[0],
        full_weight.at[0],
        weight_sems.at[0],
        weight_sems.at[1],
        device_id={"tp": last},
    )
    pl.when(core != last)(weight_push.start)

    for step in range(ring - 1):
        source = target(step)
        pltpu.make_async_remote_copy(
            part_buf.at[step],
            part_recv.at[source],
            part_send_sem.at[step],
            part_recv_sem.at[source],
            device_id={"kv": source},
        ).wait_recv()
    columns, _ = weigh(
        [local_stats] + [unpack(target(step)) + gate_stats for step in range(ring - 1)]
    )
    for inner in range(chunk):
        span = slice(inner * seq_rows, (inner + 1) * seq_rows)
        mixed = mix(
            columns,
            inner,
            [local_parts[inner]]
            + [part_recv[target(step), span, :].astype(jnp.float32) for step in range(ring - 1)],
        ).astype(jnp.bfloat16)
        for head in range(heads):
            att_buf[
                core,
                me,
                inner * nodes : (inner + 1) * nodes,
                head * head_size : (head + 1) * head_size,
            ] = mixed[head * nodes : (head + 1) * nodes, :]
    att_sends = []
    for step in reversed(range(ring - 1)):
        copy = pltpu.make_async_remote_copy(
            att_buf.at[core, me],
            att_buf.at[core, me],
            att_send_sem.at[step],
            att_recv_sem.at[core, me],
            device_id={"kv": target(step), "tp": last},
        )
        copy.start()
        att_sends.append(copy)
    local_send = pltpu.make_async_remote_copy(
        att_buf.at[0, me],
        att_buf.at[0, me],
        local_send_sem,
        att_recv_sem.at[0, me],
        device_id={"tp": last},
    )
    pl.when(core != last)(local_send.start)

    origins = [me] + [target(step) for step in range(ring - 1)]
    half_sends = [
        pltpu.make_async_remote_copy(
            half_send.at[spot],
            half_recv.at[spot],
            half_send_sem.at[spot],
            half_recv_sem.at[spot],
            device_id={"tp": partner},
        )
        for spot in range(ring)
    ]

    @pl.when(core == last)
    def _():
        weight_push.wait_recv()
        for spot, origin in enumerate(origins):
            for other in range(pair):
                if spot == 0 and other == last:
                    continue
                pltpu.make_async_remote_copy(
                    att_buf.at[other, origin],
                    att_buf.at[other, origin],
                    local_send_sem,
                    att_recv_sem.at[other, origin],
                    device_id={"tp": partner},
                ).wait_recv()
            for half in range(pair):
                columns = slice(half * half_cols, (half + 1) * half_cols)
                total = None
                for other in range(pair):
                    term = plain_dot(att_buf[other, origin], full_weight[other, :, columns])
                    term = term.astype(jnp.bfloat16).astype(jnp.float32)
                    total = term if total is None else total + term
                if half == last:
                    out_ref[origin] = total.astype(jnp.bfloat16)
                else:
                    half_send[spot] = total.astype(jnp.bfloat16)
                    half_sends[spot].start()

    @pl.when(core != last)
    def _():
        for spot, origin in enumerate(origins):
            half_sends[spot].wait_recv()
            out_ref[origin] = half_recv[spot]
        weight_push.wait_send()
        local_send.wait_send()

    for copy in sends + att_sends:
        copy.wait_send()

    @pl.when(core == last)
    def _():
        for copy in half_sends:
            copy.wait_send()


def fused(
    ring,
    pair,
    tokens,
    norm_gain,
    query_weight,
    key_weight,
    value_weight,
    forget_weight,
    forget_bias,
    query_gain,
    key_gain,
    output_weight,
    cache_keys,
    cache_values,
    cache_logcum,
    pending_keys,
    pending_values,
    pending_logcum,
    lengths,
    accepted,
    parents,
):
    seqs, nodes, width = tokens.shape
    head_size = query_gain.shape[0]
    query_cols = query_weight.shape[1]
    heads = query_cols // head_size
    block_len = cache_keys.shape[1]
    rows = seqs * nodes
    half_cols = output_weight.shape[1] // pair
    chunk = seqs // ring
    chunk_rows = chunk * nodes
    part_rows = chunk_rows * heads
    pieces = TOKEN_PIECES if rows % (64 * TOKEN_PIECES) == 0 else 1
    arrays = {
        "tokens": tokens.reshape(rows, width),
        "norm_gain": norm_gain.reshape(1, width),
        "query_weight": query_weight,
        "query_gain": query_gain.reshape(1, head_size),
        "lengths": lengths,
        "cache_log": jnp.swapaxes(cache_logcum, 1, 2),
        "cache_keys": cache_keys.reshape(seqs, block_len, head_size),
        "cache_values": cache_values.reshape(seqs, block_len, head_size),
        "parents": parents,
        "forget": forget_weight.T,
        "forget_bias": forget_bias.reshape(1, -1),
        "accepted": accepted,
        "pend_log": jnp.transpose(pending_logcum, (1, 2, 0)),
        "key_weight": key_weight,
        "value_weight": value_weight,
        "key_gain": key_gain.reshape(1, head_size),
        "pend_keys": pending_keys.reshape(-1, head_size),
        "pend_values": pending_values.reshape(-1, head_size),
        "output_weight": output_weight,
    }
    scalars = ("lengths", "accepted", "pend_log")
    joined_loads = ("query_weight", "key_weight", "value_weight", "output_weight")
    names = tuple(name for name in arrays if name not in joined_loads) + joined_loads
    order = tuple(arrays)
    held = [
        (pltpu.SMEM if name in scalars else pltpu.VMEM)(arrays[name].shape, arrays[name].dtype)
        for name in names
        if name not in joined_loads
    ]
    low, wide = jnp.bfloat16, jnp.float32
    sems = pltpu.SemaphoreType.DMA
    result = pl.pallas_call(
        functools.partial(fused_kernel, ring, pair, pieces, names, order),
        out_shape=pltpu.VMEM((ring, chunk_rows, half_cols), low),
        in_specs=[pl.BlockSpec(memory_space=pltpu.HBM)] * len(names),
        out_specs=pl.BlockSpec(memory_space=pltpu.VMEM),
        scratch_shapes=held
        + [
            pltpu.VMEM((width, query_cols + 2 * head_size), low),
            pltpu.VMEM((rows, width), low),
            pltpu.VMEM((seqs, heads, nodes, head_size), low),
            pltpu.VMEM((ring - 1, part_rows + 2 * STAT_ROWS, head_size), low),
            pltpu.VMEM((ring, part_rows + 2 * STAT_ROWS, head_size), low),
            pltpu.VMEM((pair, query_cols, pair * half_cols), low),
            pltpu.VMEM((pair, ring, chunk_rows, query_cols), low),
            pltpu.VMEM((ring, chunk_rows, half_cols), low),
            pltpu.VMEM((ring, chunk_rows, half_cols), low),
            sems((len(names),)),
            sems((pieces,)),
            sems((ring - 1,)),
            sems((ring,)),
            sems((ring - 1,)),
            sems((pair, ring)),
            sems((ring,)),
            sems((ring,)),
            sems,
            sems((2,)),
        ],
        compiler_params=pltpu.CompilerParams(
            collective_id=0, has_side_effects=True, vmem_limit_bytes=VMEM_LIMIT
        ),
    )(*[arrays[name] for name in names])
    return result.reshape(seqs, nodes, half_cols)


def layer(ring, pair, *arrays):
    tokens, output_weight, cache_keys = arrays[0], arrays[9], arrays[10]
    seqs, nodes = tokens.shape[:2]
    head_size = arrays[7].shape[0]
    heads = arrays[2].shape[1] // head_size
    fits = (
        ring > 1
        and pair == 2
        and head_size == LANES
        and cache_keys.shape[2] == 1
        and cache_keys.shape[1] % LANES == 0
        and nodes % 16 == 0
        and LANES % (heads * nodes) == 0
        and heads % 2 == 0
        and seqs % ring == 0
        and (seqs // ring * heads * nodes) % LANES == 0
        and STAT_ROWS * (ring + 1) <= LANES
        and STAT_PARTS * (seqs // ring * heads * nodes // LANES) <= 2 * STAT_ROWS
        and seqs // ring * nodes + seqs * arrays[13].shape[1] == LANES
        and (seqs * nodes) % LANES == 0
        and output_weight.shape[1] % (pair * LANES) == 0
    )
    if fits:
        return fused(ring, pair, *arrays)
    return shards(*arrays)


def solution(mesh):
    placed = (
        P("dp", None, None),
        P(),
        P(None, "tp"),
        P(None, "tp"),
        P(None, "tp"),
        P(),
        P(),
        P(),
        P(),
        P("tp", "kv"),
        P("dp", "kv", "tp", None),
        P("dp", "kv", "tp", None),
        P("dp", "kv", "tp"),
        P("dp", None, "tp", None),
        P("dp", None, "tp", None),
        P("dp", None, "tp"),
        P("dp"),
        P("dp"),
        P("dp", None),
    )
    return jax.shard_map(
        functools.partial(layer, mesh.shape["kv"], mesh.shape["tp"]), mesh=mesh, in_specs=placed, out_specs=P("dp", None, ("kv", "tp")), check_vma=False
    )
```
